32 devices in a mesh: grp: 2 (over y), kv: 4 (over z), tp: 4 (over x, core).
Axes of the slice: x: 2, y: 2, z: 4, core: 2. Of those that a mesh axis runs over, the one named last changes fastest.
Arguments:
- tokens: bfloat16 [512, 8, 4096], P('kv', 'grp'), parts along dimension 1, may hold values from -72 to 72
- lengths: int32 [8], P('grp'), parts along dimension 0, may hold values from 1 to 512, 768 in all
- chosen: int32 [8, 32, 8, 8], P('grp', 'tp', 'kv'), parts along dimension 0, may hold values from -1 to 7, as said below
- w_query: bfloat16 [4096, 2048], P(None, 'tp'), may hold values from -0.09375 to 0.09375
- w_key: bfloat16 [4096, 2048], P(None, 'tp'), may hold values from -0.09375 to 0.09375
- w_value: bfloat16 [4096, 2048], P(None, 'tp'), may hold values from -0.09375 to 0.09375
- w_gate: bfloat16 [4096, 2, 32], P(None, None, 'tp'), may hold values from -0.09375 to 0.09375
- pool_weights: float32 [2, 32, 64], replicated, may hold values from -1 to 1
- w_out: bfloat16 [2048, 4096], P(None, 'tp'), may hold values from -0.5 to 0.5
Outputs:
- mixed: bfloat16 [512, 8, 4096], P(('kv', 'tp'), 'grp'), parts along dimension 1
The draws below stay inside these ranges and needn't reach their ends.
There are 2 independent parts, one for each index of `grp`. The reference program is written for one: setup_inputs(seed, part) draws one part's arguments, and reference() takes and returns one part's arrays. A program takes and returns all parts, laid end to end along the dimension named above; an argument that names none is the same for every part. Nothing has to cross between parts.
Inputs may be any that keep to these rules, and one draw needn't show every extreme that they name: `chosen`: for query block b the live slots hold min(8, b+1) distinct blocks, all <= b, among them b, b-1 (when b >= 1) and 0; the other slots are -1.
All inputs are finite; a program needn't handle non-finite values.
Results may differ from the reference program's by a relative error of at most 0.014.
Values may be sent and summed in bfloat16 or wider, within the bound.
A program may use at most 128 MiB of HBM per device.

```python
import math
import jax
import jax.numpy as jnp
import numpy as np
from jax import lax

D = 4096
HEADS = 32
HD = 64
QB = 64
L_CMP = 32
TOP = 8
SEQS = 4
SEQ_LEN = 512
N_TP = 4


def draw_tokens(key, part):
    base = jnp.clip(jax.random.normal(key, (SEQ_LEN, SEQS, D), jnp.float32), -6.0, 6.0)
    return base.astype(jnp.bfloat16)


def draw_chosen(key, part):
    block_count = SEQ_LEN // QB
    noise = jax.random.randint(key, (SEQS, HEADS, block_count, block_count), 0, 1024)
    favored = jax.random.randint(jax.random.fold_in(key, 1), (SEQS, HEADS, 1, block_count), 0, 4)
    priority = noise + (favored == 0).astype(jnp.int32) * 2048
    query_blk = jnp.arange(block_count)[:, None]
    key_blk = jnp.arange(block_count)[None, :]
    forced = (key_blk == query_blk) | (key_blk == query_blk - 1) | (key_blk == 0)
    priority = jnp.where(forced, 8192, priority)
    priority = jnp.where(key_blk <= query_blk, priority + 1, 0)
    ranking = priority * block_count + (block_count - 1 - key_blk)
    top_scores, top_index = lax.top_k(ranking, TOP)
    live_slot = jnp.arange(TOP)[None, :] < jnp.minimum(jnp.arange(block_count) + 1, TOP)[:, None]
    return jnp.where(live_slot[None, None], top_index, -1).astype(jnp.int32)


def block_levels(key, shape, pieces, smallest, largest):
    loudness = 1.0
    for axis_at, blocks in pieces:
        heights = jax.random.uniform(jax.random.fold_in(jax.random.fold_in(key, 6), axis_at), (blocks,), jnp.float32, smallest / len(pieces), largest / len(pieces))
        loudness = loudness * jnp.repeat(jnp.exp(heights), shape[axis_at] // blocks).reshape((-1,) + (1,) * (len(shape) - 1 - axis_at))
    return loudness


def length_profile(amount, total, reach, skew):
    weights = [(1 << 20) // math.isqrt(rank ** skew) + 1 for rank in range(2, amount + 1)]
    rest, counts = total - reach - (amount - 1), [1] * (amount - 1)
    while rest > 0:
        candidates = [i for i in range(amount - 1) if counts[i] < reach]
        mass, remaining = sum([weights[i] for i in candidates]), rest
        for i in candidates:
            more = min(reach - counts[i], max(1, remaining * weights[i] // mass), rest)
            counts[i] = counts[i] + more
            rest = rest - more
    return np.array([reach] + counts)


def uneven_parts(rng, number_of, total, most, lean):
    if number_of == 2:
        one = jax.random.randint(rng, (), max(1, total - most), min(most, total - 1) + 1)
        return jnp.stack([one, total - one])
    sizes = jnp.asarray(length_profile(number_of, total, most, lean), jnp.int32)
    couples = (number_of - 1) // 2
    giver, sink = sizes[1:1 + 2 * couples:2], sizes[2:2 + 2 * couples:2]
    slack = jnp.minimum(giver - 1, most - sink)
    moved = jax.random.randint(jax.random.fold_in(rng, 1), (couples,), 0, 1 << 20) % (slack + 1)
    sizes = sizes.at[1:1 + 2 * couples:2].set(giver - moved).at[2:2 + 2 * couples:2].set(sink + moved)
    return sizes[jax.random.permutation(jax.random.fold_in(rng, 2), number_of)]


def scatter_about(own_key, dims, width, bound, split=(), dtype=jnp.bfloat16):
    result = jax.random.normal(own_key, dims, jnp.float32) * width
    if len(split) > 0:
        result = block_levels(own_key, dims, split, -0.22, 0.18) * result
    return jnp.clip(result, min=-bound, max=bound).astype(dtype)


def setup_inputs(seed: int = 0, part: int = 0) -> dict:
    keys = jax.random.split(jax.random.key(seed), 10)
    part_splits = jax.random.split(jax.random.fold_in(keys[9], part), 10)
    return {
        "tokens": draw_tokens(jax.random.fold_in(jax.random.fold_in(keys[9], part), 71), part),
        "lengths": uneven_parts(part_splits[1], SEQS, SEQS * SEQ_LEN * 3 // 8, SEQ_LEN, 2).astype(jnp.int32),
        "chosen": draw_chosen(jax.random.fold_in(jax.random.fold_in(keys[9], part), 71), part),
        "w_query": scatter_about(keys[3], (D, HEADS * HD), D ** -0.5, 0.09375, ((1, 4),)),
        "w_key": scatter_about(keys[4], (D, HEADS * HD), D ** -0.5, 0.09375, ((1, 4),)),
        "w_value": scatter_about(keys[5], (D, HEADS * HD), D ** -0.5, 0.09375, ((1, 4),)),
        "w_gate": scatter_about(keys[6], (D, 2, HEADS), D ** -0.5, 0.09375, ((2, 4),)),
        "pool_weights": scatter_about(keys[7], (2, L_CMP, HD), L_CMP ** -0.5, 1.0, (), jnp.float32),
        "w_out": scatter_about(keys[8], (HEADS * HD, D), (HEADS * HD // 16) ** -0.5, 0.5, ((1, 4),)),
    }


LOW_FILL = -1e30


def rounded(value):
    return lax.optimization_barrier(value.astype(jnp.bfloat16)).astype(jnp.float32)


def head_attend(queries, key_rows, value_rows, chosen, pool_weights, lengths):
    seq_len, seq_count, head_dim = queries.shape
    score_scale = head_dim ** -0.5
    query_pos = jnp.arange(seq_len)
    cmp_count = seq_len // L_CMP
    key_pooled = rounded((key_rows.reshape(cmp_count, L_CMP, seq_count, head_dim) * pool_weights[0][None, :, None, :]).sum(1))
    val_pooled = rounded((value_rows.reshape(cmp_count, L_CMP, seq_count, head_dim) * pool_weights[1][None, :, None, :]).sum(1))
    cmp_end = jnp.arange(cmp_count) * L_CMP + L_CMP - 1
    scores = jnp.einsum('qsd,csd->sqc', queries, key_pooled) * score_scale
    usable = (cmp_end[None, None, :] <= query_pos[None, :, None]) & (cmp_end[None, None, :] < lengths[:, None, None])
    row_top = jnp.max(jnp.where(usable, scores, LOW_FILL), axis=-1, keepdims=True)
    weights = jnp.where(usable, jnp.exp(scores - row_top), 0.0)
    totals = jnp.sum(weights, axis=-1)
    pooled_out = jnp.einsum('sqc,csd->sqd', rounded(weights), val_pooled) / jnp.where(totals > 0, totals, 1.0)[..., None]
    block_count = seq_len // QB
    key_table = key_rows.reshape(block_count, QB, seq_count, head_dim).transpose(2, 0, 1, 3)
    val_table = value_rows.reshape(block_count, QB, seq_count, head_dim).transpose(2, 0, 1, 3)
    clipped = jnp.maximum(chosen, 0)
    index = clipped[:, :, :, None, None]
    key_sel = jnp.take_along_axis(key_table[:, None], index, axis=2).reshape(seq_count, block_count, TOP * QB, head_dim)
    val_sel = jnp.take_along_axis(val_table[:, None], index, axis=2).reshape(seq_count, block_count, TOP * QB, head_dim)
    query_blocks = queries.transpose(1, 0, 2).reshape(seq_count, block_count, QB, head_dim)
    scores = jnp.einsum('sbqd,sbkd->sbqk', query_blocks, key_sel) * score_scale
    key_pos = (clipped[..., None] * QB + jnp.arange(QB)).reshape(seq_count, block_count, TOP * QB)
    live_key = jnp.repeat(chosen >= 0, QB, axis=-1)
    block_pos = query_pos.reshape(block_count, QB)
    usable = live_key[:, :, None, :] & (key_pos[:, :, None, :] <= block_pos[None, :, :, None]) & (key_pos[:, :, None, :] < lengths[:, None, None, None])
    row_top = jnp.max(jnp.where(usable, scores, LOW_FILL), axis=-1, keepdims=True)
    weights = jnp.where(usable, jnp.exp(scores - row_top), 0.0)
    totals = jnp.sum(weights, axis=-1)
    picked_out = jnp.einsum('sbqk,sbkd->sbqd', rounded(weights), val_sel) / jnp.where(totals > 0, totals, 1.0)[..., None]
    return pooled_out, picked_out.reshape(seq_count, seq_len, head_dim)


def reference(tokens, lengths, chosen, w_query, w_key, w_value, w_gate, pool_weights, w_out):
    seq_len, seq_count, model_width = tokens.shape
    head_count = w_query.shape[1] // HD
    flat_rows = tokens.reshape(seq_len * seq_count, model_width)

    def project(weight):
        product = jnp.dot(flat_rows, weight, preferred_element_type=jnp.float32)
        return rounded(product).reshape(seq_len, seq_count, head_count, HD).transpose(2, 0, 1, 3)

    queries = project(w_query)
    key_rows = project(w_key)
    value_rows = project(w_value)
    gate_values = jax.nn.sigmoid(jnp.dot(flat_rows, w_gate.reshape(model_width, 2 * head_count), preferred_element_type=jnp.float32))
    gate_values = gate_values.reshape(seq_len, seq_count, 2, head_count)

    def one_head(inputs):
        return head_attend(inputs[0], inputs[1], inputs[2], inputs[3], pool_weights, lengths)

    pooled_out, picked_out = lax.map(one_head, (queries, key_rows, value_rows, chosen.transpose(1, 0, 2, 3)))
    combined = gate_values[:, :, 0, :, None] * pooled_out.transpose(2, 1, 0, 3) + gate_values[:, :, 1, :, None] * picked_out.transpose(2, 1, 0, 3)
    live = jnp.arange(seq_len)[:, None] < lengths[None, :]
    attended = jnp.where(live[:, :, None, None], combined, 0.0).astype(jnp.bfloat16).reshape(seq_len * seq_count, head_count * HD)
    part_width = head_count * HD // N_TP
    summed = jnp.zeros((seq_len * seq_count, model_width), jnp.float32)
    for shard in range(N_TP):
        product = jnp.dot(attended[:, shard * part_width:(shard + 1) * part_width], w_out[shard * part_width:(shard + 1) * part_width], preferred_element_type=jnp.float32)
        summed = summed + rounded(product)
    return summed.astype(jnp.bfloat16).reshape(seq_len, seq_count, model_width)
```

```python
import functools

import jax
import jax.numpy as jnp
from jax import lax
from jax.experimental import pallas as pl
from jax.experimental.pallas import tpu as pltpu
from jax.sharding import PartitionSpec as P

HD = 64
QB = 64
L_CMP = 32
PAD = 16
LOW = -1e30
FLOOR = -1e29
MESH = pl.DeviceIdType.MESH
NT = (((1,), (1,)), ((), ()))


def rank_slots(seq_count, seq_len, rows, shards):
    total = seq_count * seq_len * 3 // 8
    slots = []
    for r in range(seq_count):
        most = min(seq_len, (total - (seq_count - 1 - r)) // (r + 1))
        slots.append(min(shards, -(-most // rows)))
    return slots


def project_kernel(
    rank_ref, len_ref, base_ref, x_ref, wq_ref, wk_ref, wv_ref, wg_ref, pool_ref,
    q_ref, kv_ref, g_ref, acc, gacc,
):
    step = pl.program_id(0)
    width = wq_ref.shape[1]
    x = x_ref[...]

    @pl.when(step == 0)
    def _():
        acc[...] = jnp.zeros_like(acc)
        gacc[...] = jnp.zeros_like(gacc)

    for n, w in enumerate((wq_ref, wk_ref, wv_ref)):
        acc[:, n * width : (n + 1) * width] += jnp.dot(
            x, w[...], preferred_element_type=jnp.float32
        )
    gacc[...] += jnp.dot(x, wg_ref[...], preferred_element_type=jnp.float32)

    @pl.when(step == pl.num_programs(0) - 1)
    def _():
        seqs, rows, _ = q_ref.shape
        pool = pool_ref[...]
        for s in range(seqs):
            at = rank_ref[s]
            span = slice(s * rows, (s + 1) * rows)
            q = acc[span, :width].astype(jnp.bfloat16)
            q_ref[at] = q * jnp.bfloat16(HD**-0.5)
            kv = acc[span, width:].astype(jnp.bfloat16)
            kv_ref[at, :rows, :] = kv
            grouped = kv.astype(jnp.float32).reshape(rows // L_CMP, L_CMP, 2 * width)
            pooled = (grouped * pool[None]).sum(1)
            fill = jnp.zeros((PAD - rows // L_CMP, 2 * width), jnp.float32)
            kv_ref[at, rows:, :] = jnp.concatenate([pooled, fill], 0).astype(jnp.bfloat16)
            gate = jax.nn.sigmoid(gacc[span, :])
            pos = base_ref[0] + lax.broadcasted_iota(jnp.int32, gate.shape, 0)
            g_ref[at] = jnp.where(pos < len_ref[s], gate, 0.0)


def mixer_kernel(
    slots, shards, ntp,
    q_ref, kv_ref, g_ref, bias_ref, pbias_ref, w_hbm,
    out_ref,
    items, att, mixed, pools, acc, top, tot, w_vmem,
    w_sem, z_send, z_recv, a_send, a_recv, o_send, o_recv,
):
    seqs, rows, width = q_ref.shape
    heads = width // HD
    pairs = heads // 2
    blocks = rows // QB
    chips = ntp // 2
    col = w_hbm.shape[1]
    part = rows // ntp
    i = lax.axis_index("kv")
    t = lax.axis_index("tp")
    x, c = t // 2, t % 2
    mate = x * 2 + (1 - c)

    w_copy = pltpu.make_async_copy(w_hbm, w_vmem, w_sem)
    w_copy.start()
    pools[...] = jnp.zeros_like(pools)

    def active(shard):
        count = 0
        for n in slots:
            count = count + jnp.where(shard < n, 1, 0)
        return count

    mine = active(i)
    after = active(i + 1)

    barrier = pltpu.get_barrier_semaphore()
    for d in range(1, ntp):
        pl.semaphore_signal(
            barrier, inc=1, device_id={"tp": lax.rem(t + d, ntp)}, device_id_type=MESH
        )

    @pl.when(i > 0)
    def _():
        pl.semaphore_signal(barrier, inc=1, device_id={"kv": i - 1}, device_id_type=MESH)

    @pl.when(i < shards - 1)
    def _():
        pl.semaphore_signal(barrier, inc=1, device_id={"kv": i + 1}, device_id_type=MESH)

    expected = ntp - 1 + jnp.where(i > 0, 1, 0) + jnp.where(i < shards - 1, 1, 0)
    pl.semaphore_wait(barrier, expected)

    def own_copy(r):
        return pltpu.make_async_remote_copy(
            src_ref=kv_ref.at[r], dst_ref=items.at[r, i],
            send_sem=z_send.at[r, i], recv_sem=z_recv.at[r, i],
            device_id={"kv": i + 1}, device_id_type=MESH,
        )

    def relay_copy(r, j):
        return pltpu.make_async_remote_copy(
            src_ref=items.at[r, j], dst_ref=items.at[r, j],
            send_sem=z_send.at[r, j], recv_sem=z_recv.at[r, j],
            device_id={"kv": i + 1}, device_id_type=MESH,
        )

    def block_copy(r, k, block, target):
        return pltpu.make_async_remote_copy(
            src_ref=att.at[r, block], dst_ref=att.at[r, block],
            send_sem=a_send.at[r, k], recv_sem=a_recv.at[r, k],
            device_id={"tp": target}, device_id_type=MESH,
        )

    def side(d):
        return lax.rem(x + d, chips) * 2 + c

    def origin(d):
        return lax.rem(x + chips - d, chips) * 2

    def out_copy(r, d):
        target = lax.rem(t + d, ntp)
        return pltpu.make_async_remote_copy(
            src_ref=mixed.at[r, pl.ds(pl.multiple_of(target * part, part), part), :],
            dst_ref=out_ref.at[r, :, pl.ds(pl.multiple_of(t * col, col), col)],
            send_sem=o_send.at[r, d], recv_sem=o_recv.at[r, d],
            device_id={"tp": target}, device_id_type=MESH,
        )

    def send_own(r, carry):
        own_copy(r).start()
        return carry

    lax.fori_loop(0, after, send_own, 0)

    lane = lax.broadcasted_iota(jnp.int32, (rows, 2 * HD), 1)
    first = lane < HD

    def pair_queries(r, p):
        q = q_ref[r, :, p * 2 * HD : (p + 1) * 2 * HD]
        zero = jnp.zeros_like(q)
        return jnp.concatenate([jnp.where(first, q, zero), jnp.where(first, zero, q)], 0)

    def scores_of(r, p, keys, bias):
        scores = lax.dot_general(
            pair_queries(r, p), keys, NT, preferred_element_type=jnp.float32
        )
        return scores + bias

    def block_bias(r, j, p):
        lines = [
            jnp.broadcast_to(bias_ref[r, j, n : n + 1, :], (QB, rows))
            for n in range(p * 2 * blocks, (p + 1) * 2 * blocks)
        ]
        return jnp.concatenate(lines, 0)

    def columns(p):
        return slice(p * 2 * HD, (p + 1) * 2 * HD)

    def value_columns(p):
        return slice(width + p * 2 * HD, width + (p + 1) * 2 * HD)

    def attend(r):
        row = lax.broadcasted_iota(jnp.int32, (2 * rows, rows), 0)
        row = jnp.where(row >= rows, row - rows, row)
        key = lax.broadcasted_iota(jnp.int32, (2 * rows, rows), 1)
        causal = jnp.where(key <= row, 0.0, LOW)
        pools[pl.ds(pl.multiple_of(i * PAD, PAD), PAD), :] = kv_ref[r, rows:, :]
        for p in range(pairs):
            bias = block_bias(r, i, p) + causal
            scores = scores_of(r, p, kv_ref[r, :rows, columns(p)], bias)
            peak = jnp.maximum(jnp.max(scores, axis=1, keepdims=True), FLOOR)
            e = jnp.exp(scores - peak)
            top[p] = jnp.broadcast_to(peak, (2 * rows, 2 * HD))
            tot[p] = jnp.broadcast_to(jnp.sum(e, axis=1, keepdims=True), (2 * rows, 2 * HD))
            acc[p] = jnp.dot(
                e.astype(jnp.bfloat16), kv_ref[r, :rows, value_columns(p)],
                preferred_element_type=jnp.float32,
            )

        def chunk(j, carry):
            pools[pl.ds(pl.multiple_of(j * PAD, PAD), PAD), :] = items[r, j, rows:, :]
            for p in range(pairs):
                scores = scores_of(
                    r, p, items[r, j, :rows, columns(p)], block_bias(r, j, p)
                )
                old = top[p]
                peak = jnp.maximum(old, jnp.max(scores, axis=1, keepdims=True))
                shrink = jnp.exp(old - peak)
                e = jnp.exp(scores - peak[:, :1])
                top[p] = peak
                tot[p] = tot[p] * shrink + jnp.sum(e, axis=1, keepdims=True)
                acc[p] = acc[p] * shrink + jnp.dot(
                    e.astype(jnp.bfloat16), items[r, j, :rows, value_columns(p)],
                    preferred_element_type=jnp.float32,
                )
            return carry

        lax.fori_loop(0, i, chunk, 0)

        pbias = pbias_ref[r]
        pbias = jnp.concatenate([pbias, pbias], 0)
        for p in range(pairs):
            scores = scores_of(r, p, pools[:, columns(p)], pbias)
            peak = jnp.maximum(jnp.max(scores, axis=1, keepdims=True), FLOOR)
            e = jnp.exp(scores - peak)
            total = jnp.sum(e, axis=1, keepdims=True)
            pooled = jnp.dot(
                e.astype(jnp.bfloat16), pools[:, value_columns(p)],
                preferred_element_type=jnp.float32,
            ) / jnp.where(total > 0, total, 1.0)
            picked_total = tot[p]
            picked = acc[p] / jnp.where(picked_total > 0, picked_total, 1.0)
            halves = []
            for side_at in range(2):
                h = 2 * p + side_at
                span = slice(side_at * rows, (side_at + 1) * rows)
                halves.append(
                    g_ref[r, :, h : h + 1] * pooled[span]
                    + g_ref[r, :, heads + h : heads + h + 1] * picked[span]
                )
            att[r, t, :, columns(p)] = jnp.where(first, halves[0], halves[1]).astype(
                jnp.bfloat16
            )

    def step(r, carry):
        @pl.when(r < mine)
        def _():
            def arrive(n, inner):
                j = i - 1 - n
                relay_copy(r, j).wait_recv()

                @pl.when(r < after)
                def _():
                    relay_copy(r, j).start()

                return inner

            lax.fori_loop(0, i, arrive, 0)
            attend(r)
            for d in range(1, chips):
                block_copy(r, d, t, side(d)).start()
            block_copy(r, 0, t, mate).start()

        @pl.when(r >= 1)
        def _():
            b = r - 1
            for d in range(1, chips):
                block_copy(b, d, origin(d) + c, mate).wait_recv()
                block_copy(b, chips - 1 + d, origin(d) + c, mate).start()
            block_copy(b, 0, mate, mate).wait_recv()
            for d in range(1, chips):
                block_copy(b, chips - 1 + d, origin(d) + 1 - c, mate).wait_recv()

            @pl.when(r == 1)
            def _():
                w_copy.wait()

            total = jnp.dot(att[b, 0], w_vmem[:width, :], preferred_element_type=jnp.float32)
            for g in range(1, ntp):
                total = total + jnp.dot(
                    att[b, g], w_vmem[g * width : (g + 1) * width, :],
                    preferred_element_type=jnp.float32,
                )
            mixed[b] = total.astype(jnp.bfloat16)
            for d in range(1, ntp):
                out_copy(b, d).start()
            out_ref[b, :, pl.ds(pl.multiple_of(t * col, col), col)] = mixed[
                b, pl.ds(pl.multiple_of(t * part, part), part), :
            ]

        return carry

    lax.fori_loop(0, mine + 1, step, 0)

    def blank(r, carry):
        out_ref[r] = jnp.zeros(out_ref.shape[1:], out_ref.dtype)
        return carry

    lax.fori_loop(mine, seqs, blank, 0)

    def finish(r, carry):
        for d in range(1, ntp):
            out_copy(r, d).wait_send()
            source = lax.rem(t + ntp - d, ntp)
            pltpu.make_async_remote_copy(
                src_ref=mixed.at[r, :part, :],
                dst_ref=out_ref.at[r, :, pl.ds(pl.multiple_of(source * col, col), col)],
                send_sem=o_send.at[r, d], recv_sem=o_recv.at[r, d],
                device_id={"tp": source}, device_id_type=MESH,
            ).wait_recv()
        block_copy(r, 0, t, mate).wait_send()
        for d in range(1, chips):
            block_copy(r, d, t, side(d)).wait_send()
            block_copy(r, chips - 1 + d, origin(d) + c, mate).wait_send()
        return carry

    lax.fori_loop(0, mine, finish, 0)

    def sent(r, carry):
        own_copy(r).wait_send()

        def relayed(j, inner):
            relay_copy(r, j).wait_send()
            return inner

        lax.fori_loop(0, i, relayed, 0)
        return carry

    lax.fori_loop(0, after, sent, 0)


def body(tokens, lengths, chosen, w_query, w_key, w_value, w_gate, pool_weights, w_out):
    rows, seqs, model = tokens.shape
    width = w_query.shape[1]
    heads = width // HD
    col = w_out.shape[1]
    shards = lax.axis_size("kv")
    ntp = lax.axis_size("tp")
    shard = lax.axis_index("kv")
    base = (shard * rows).astype(jnp.int32)
    blocks = rows // QB
    slots = rank_slots(seqs, rows * shards, rows, shards)

    ids = jnp.arange(seqs)
    ahead = (lengths[None, :] > lengths[:, None]) | (
        (lengths[None, :] == lengths[:, None]) & (ids[None, :] < ids[:, None])
    )
    rank = jnp.sum(ahead.astype(jnp.int32), axis=1)
    order = rank[None, :] == ids[:, None]
    sorted_len = jnp.sum(jnp.where(order, lengths[None, :], 0), axis=1)
    ranked = jnp.sum(jnp.where(order[:, :, None, None, None], chosen[None], 0), axis=1)

    block_ids = jnp.arange(shards * blocks)
    picked = jnp.any(ranked[..., None] == block_ids, axis=3)
    picked = picked.reshape(seqs, heads * blocks, shards, blocks).transpose(0, 2, 1, 3)
    picked = jnp.repeat(picked, QB, axis=3)
    key_pos = (jnp.arange(shards) * rows)[:, None] + jnp.arange(rows)[None, :]
    near = key_pos[None, :, None, :] < sorted_len[:, None, None, None]
    bias = jnp.where(picked & near, 0.0, LOW).astype(jnp.float32)

    slot = jnp.arange(shards * PAD)
    inner = slot % PAD
    end = (slot // PAD) * rows + inner * L_CMP + L_CMP - 1
    pos = base + jnp.arange(rows)
    usable = (
        (inner < rows // L_CMP)[None, None, :]
        & (end[None, None, :] <= pos[None, :, None])
        & (end[None, None, :] < sorted_len[:, None, None])
    )
    pbias = jnp.where(usable, 0.0, LOW).astype(jnp.float32)
    pool = jnp.concatenate(
        [jnp.tile(pool_weights[0], (1, heads)), jnp.tile(pool_weights[1], (1, heads))], 1
    )

    flat = tokens.transpose(1, 0, 2).reshape(seqs * rows, model)
    gate_w = w_gate.reshape(model, 2 * heads)
    depth = model // 8
    whole = lambda k, *_: (0, 0)
    q, kv, gates = pl.pallas_call(
        project_kernel,
        grid_spec=pltpu.PrefetchScalarGridSpec(
            num_scalar_prefetch=3,
            grid=(model // depth,),
            in_specs=[
                pl.BlockSpec((seqs * rows, depth), lambda k, *_: (0, k)),
                pl.BlockSpec((depth, width), lambda k, *_: (k, 0)),
                pl.BlockSpec((depth, width), lambda k, *_: (k, 0)),
                pl.BlockSpec((depth, width), lambda k, *_: (k, 0)),
                pl.BlockSpec((depth, 2 * heads), lambda k, *_: (k, 0)),
                pl.BlockSpec((L_CMP, 2 * width), whole),
            ],
            out_specs=[
                pl.BlockSpec((seqs, rows, width), lambda k, *_: (0, 0, 0)),
                pl.BlockSpec((seqs, rows + PAD, 2 * width), lambda k, *_: (0, 0, 0)),
                pl.BlockSpec((seqs, rows, 2 * heads), lambda k, *_: (0, 0, 0)),
            ],
            scratch_shapes=[
                pltpu.VMEM((seqs * rows, 3 * width), jnp.float32),
                pltpu.VMEM((seqs * rows, 2 * heads), jnp.float32),
            ],
        ),
        out_shape=[
            jax.ShapeDtypeStruct((seqs, rows, width), jnp.bfloat16),
            jax.ShapeDtypeStruct((seqs, rows + PAD, 2 * width), jnp.bfloat16),
            jax.ShapeDtypeStruct((seqs, rows, 2 * heads), jnp.float32),
        ],
        compiler_params=pltpu.CompilerParams(vmem_limit_bytes=48 * 2**20),
    )(rank, lengths, base[None], flat, w_query, w_key, w_value, gate_w, pool)

    chips = ntp // 2
    vmem = pl.BlockSpec(memory_space=pltpu.VMEM)
    dma = pltpu.SemaphoreType.DMA
    out = pl.pallas_call(
        functools.partial(mixer_kernel, slots, shards, ntp),
        out_shape=jax.ShapeDtypeStruct((seqs, rows // ntp, ntp * col), jnp.bfloat16),
        in_specs=[vmem] * 5 + [pl.BlockSpec(memory_space=pl.ANY)],
        out_specs=vmem,
        scratch_shapes=[
            pltpu.VMEM((seqs, shards, rows + PAD, 2 * width), jnp.bfloat16),
            pltpu.VMEM((seqs, ntp, rows, width), jnp.bfloat16),
            pltpu.VMEM((seqs, rows, col), jnp.bfloat16),
            pltpu.VMEM((shards * PAD, 2 * width), jnp.bfloat16),
            pltpu.VMEM((heads // 2, 2 * rows, 2 * HD), jnp.float32),
            pltpu.VMEM((heads // 2, 2 * rows, 2 * HD), jnp.float32),
            pltpu.VMEM((heads // 2, 2 * rows, 2 * HD), jnp.float32),
            pltpu.VMEM(w_out.shape, jnp.bfloat16),
            dma,
            dma((seqs, shards)),
            dma((seqs, shards)),
            dma((seqs, 2 * chips)),
            dma((seqs, 2 * chips)),
            dma((seqs, ntp)),
            dma((seqs, ntp)),
        ],
        compiler_params=pltpu.CompilerParams(
            collective_id=0, has_side_effects=True, vmem_limit_bytes=56 * 2**20
        ),
    )(q, kv, gates, bias, pbias, w_out)
    parts = [lax.dynamic_index_in_dim(out, rank[s], 0, keepdims=False) for s in range(seqs)]
    return jnp.stack(parts, axis=1)


def solution(mesh):
    placed = (
        P("kv", "grp", None),
        P("grp"),
        P("grp", "tp", "kv", None),
        P(None, "tp"),
        P(None, "tp"),
        P(None, "tp"),
        P(None, None, "tp"),
        P(),
        P(None, "tp"),
    )
    return jax.shard_map(
        body, mesh=mesh, in_specs=placed, out_specs=P(("kv", "tp"), "grp", None), check_vma=False
    )
```

```python
import functools

import jax
import jax.numpy as jnp
from jax import lax
from jax.experimental import pallas as pl
from jax.experimental.pallas import tpu as pltpu
from jax.sharding import PartitionSpec as P

HD = 64
QB = 64
L_CMP = 32
PAD = 16
LOW = -1e30
FLOOR = -1e29
MESH = pl.DeviceIdType.MESH
NT = (((1,), (1,)), ((), ()))


def rank_slots(seq_count, seq_len, rows, shards):
    total = seq_count * seq_len * 3 // 8
    slots = []
    for r in range(seq_count):
        most = min(seq_len, (total - (seq_count - 1 - r)) // (r + 1))
        slots.append(min(shards, -(-most // rows)))
    return slots


def mixer_kernel(
    slots, shards, ntp,
    len_ref, chosen_ref, pool_ref, wg_ref, tok_hbm, wq_hbm, wk_hbm, wv_hbm, w_hbm,
    final_ref,
    tok, xt, proj, q_ref, kv_ref, g_ref, out_ref,
    items, att, mixed, pools, acc, top, tot, wq_vmem, wk_vmem, wv_vmem, w_vmem,
    in_sem, q_sem, w_sem, z_send, z_recv, a_send, a_recv, o_send, o_recv,
):
    seqs, rows, width = q_ref.shape
    steps, _, _, depth = tok.shape
    heads = width // HD
    pairs = heads // 2
    blocks = rows // QB
    chips = ntp // 2
    col = w_hbm.shape[1]
    part = rows // ntp
    i = lax.axis_index("kv")
    t = lax.axis_index("tp")
    x, c = t // 2, t % 2
    mate = x * 2 + (1 - c)

    def span_of(k):
        return pl.ds(pl.multiple_of(k * depth, depth), depth)

    def input_copies(k):
        return (
            pltpu.make_async_copy(tok_hbm.at[:, :, span_of(k)], tok.at[k], in_sem.at[k, 0]),
            pltpu.make_async_copy(wk_hbm.at[span_of(k)], wk_vmem.at[span_of(k)], in_sem.at[k, 1]),
            pltpu.make_async_copy(wv_hbm.at[span_of(k)], wv_vmem.at[span_of(k)], in_sem.at[k, 2]),
        )

    for k in range(steps):
        for copy in input_copies(k):
            copy.start()
    q_copy = pltpu.make_async_copy(wq_hbm, wq_vmem, q_sem)
    q_copy.start()
    w_copy = pltpu.make_async_copy(w_hbm, w_vmem, w_sem)
    w_copy.start()
    pools[...] = jnp.zeros_like(pools)

    lens = [len_ref[s] for s in range(seqs)]
    ranks = []
    for s in range(seqs):
        place = jnp.int32(0)
        for o in range(seqs):
            if o != s:
                ahead = lens[o] >= lens[s] if o < s else lens[o] > lens[s]
                place = place + jnp.where(ahead, 1, 0)
        ranks.append(place)

    def seq_at(r):
        found = jnp.int32(0)
        for s in range(1, seqs):
            found = found + jnp.where(ranks[s] == r, s, 0)
        return found

    def live_at(r):
        found = jnp.int32(0)
        for s in range(seqs):
            found = found + jnp.where(ranks[s] == r, lens[s], 0)
        return found

    def active(shard):
        count = 0
        for n in slots:
            count = count + jnp.where(shard < n, 1, 0)
        return count

    mine = active(i)
    after = active(i + 1)

    barrier = pltpu.get_barrier_semaphore()
    for d in range(1, ntp):
        pl.semaphore_signal(
            barrier, inc=1, device_id={"tp": lax.rem(t + d, ntp)}, device_id_type=MESH
        )

    @pl.when(i > 0)
    def _():
        pl.semaphore_signal(barrier, inc=1, device_id={"kv": i - 1}, device_id_type=MESH)

    @pl.when(i < shards - 1)
    def _():
        pl.semaphore_signal(barrier, inc=1, device_id={"kv": i + 1}, device_id_type=MESH)

    def project(k, carry):
        for copy in input_copies(k):
            copy.wait()
        piece = jnp.swapaxes(tok[k], 0, 1).reshape(seqs * rows, depth)
        xt[k] = piece
        for n, w in enumerate((wk_vmem, wv_vmem)):
            product = jnp.dot(piece, w[span_of(k), :], preferred_element_type=jnp.float32)
            product = product.reshape(seqs, rows, width)
            span = slice(n * width, (n + 1) * width)

            @pl.when(k == 0)
            def _():
                proj[:, :, span] = product

            @pl.when(k > 0)
            def _():
                proj[:, :, span] += product

        return carry

    lax.fori_loop(0, steps, project, 0)

    def keep(r, carry):
        kv_ref[r] = proj[seq_at(r)].astype(jnp.bfloat16)
        return carry

    lax.fori_loop(0, seqs, keep, 0)
    expected = ntp - 1 + jnp.where(i > 0, 1, 0) + jnp.where(i < shards - 1, 1, 0)
    pl.semaphore_wait(barrier, expected)

    def own_copy(r):
        return pltpu.make_async_remote_copy(
            src_ref=kv_ref.at[r], dst_ref=items.at[r, i],
            send_sem=z_send.at[r, i], recv_sem=z_recv.at[r, i],
            device_id={"kv": i + 1}, device_id_type=MESH,
        )

    def relay_copy(r, j):
        return pltpu.make_async_remote_copy(
            src_ref=items.at[r, j], dst_ref=items.at[r, j],
            send_sem=z_send.at[r, j], recv_sem=z_recv.at[r, j],
            device_id={"kv": i + 1}, device_id_type=MESH,
        )

    def block_copy(r, k, block, target):
        return pltpu.make_async_remote_copy(
            src_ref=att.at[r, block], dst_ref=att.at[r, block],
            send_sem=a_send.at[r, k], recv_sem=a_recv.at[r, k],
            device_id={"tp": target}, device_id_type=MESH,
        )

    def side(d):
        return lax.rem(x + d, chips) * 2 + c

    def origin(d):
        return lax.rem(x + chips - d, chips) * 2

    def out_copy(r, d):
        target = lax.rem(t + d, ntp)
        return pltpu.make_async_remote_copy(
            src_ref=mixed.at[r, pl.ds(pl.multiple_of(target * part, part), part), :],
            dst_ref=out_ref.at[r, :, pl.ds(pl.multiple_of(t * col, col), col)],
            send_sem=o_send.at[r, d], recv_sem=o_recv.at[r, d],
            device_id={"tp": target}, device_id_type=MESH,
        )

    def send_own(r, carry):
        own_copy(r).start()
        return carry

    lax.fori_loop(0, jnp.where(i == 0, after, jnp.minimum(after, 1)), send_own, 0)

    q_copy.wait()

    def project_queries(k, carry):
        piece = xt[k]
        product = jnp.dot(piece, wq_vmem[span_of(k), :], preferred_element_type=jnp.float32)
        product = product.reshape(seqs, rows, width)
        gate = lax.dot_general(piece, wg_ref[k], NT, preferred_element_type=jnp.float32)
        gate = gate.reshape(seqs, rows, 2 * heads)

        @pl.when(k == 0)
        def _():
            proj[:, :, :width] = product
            g_ref[...] = gate

        @pl.when(k > 0)
        def _():
            proj[:, :, :width] += product
            g_ref[...] += gate

        return carry

    lax.fori_loop(0, steps, project_queries, 0)
    g_ref[...] = jax.nn.sigmoid(g_ref[...])

    def keep_queries(r, carry):
        q_ref[r] = proj[seq_at(r), :, :width].astype(jnp.bfloat16) * jnp.bfloat16(HD**-0.5)
        return carry

    lax.fori_loop(0, mine, keep_queries, 0)

    lane = lax.broadcasted_iota(jnp.int32, (rows, 2 * HD), 1)
    first = lane < HD

    def pair_queries(r, p):
        q = q_ref[r, :, p * 2 * HD : (p + 1) * 2 * HD]
        zero = jnp.zeros_like(q)
        return jnp.concatenate([jnp.where(first, q, zero), jnp.where(first, zero, q)], 0)

    def scores_of(r, p, keys, bias):
        scores = lax.dot_general(
            pair_queries(r, p), keys, NT, preferred_element_type=jnp.float32
        )
        return scores + bias

    def chunk_bias(r, j):
        listed = chosen_ref[seq_at(r)]
        key_at = j * rows + lax.broadcasted_iota(jnp.int32, (heads * blocks, rows), 1)
        key_blk = key_at // QB
        hit = listed[:, :1] == key_blk
        for n in range(1, listed.shape[1]):
            hit = hit | (listed[:, n : n + 1] == key_blk)
        return jnp.where(hit & (key_at < live_at(r)), 0.0, LOW)

    def block_bias(bias, p):
        lines = [
            jnp.broadcast_to(bias[n : n + 1, :], (QB, rows))
            for n in range(p * 2 * blocks, (p + 1) * 2 * blocks)
        ]
        return jnp.concatenate(lines, 0)

    def pool_rows(kv, j):
        grouped = kv.astype(jnp.float32).reshape(rows // L_CMP, L_CMP, 2 * width)
        pooled = (grouped * pool_ref[...][None]).sum(1)
        fill = jnp.zeros((PAD - rows // L_CMP, 2 * width), jnp.float32)
        pools[pl.ds(pl.multiple_of(j * PAD, PAD), PAD), :] = jnp.concatenate(
            [pooled, fill], 0
        ).astype(jnp.bfloat16)

    def columns(p):
        return slice(p * 2 * HD, (p + 1) * 2 * HD)

    def value_columns(p):
        return slice(width + p * 2 * HD, width + (p + 1) * 2 * HD)

    def attend(r):
        row = lax.broadcasted_iota(jnp.int32, (2 * rows, rows), 0)
        row = jnp.where(row >= rows, row - rows, row)
        key = lax.broadcasted_iota(jnp.int32, (2 * rows, rows), 1)
        causal = jnp.where(key <= row, 0.0, LOW)
        pool_rows(kv_ref[r], i)
        own_bias = chunk_bias(r, i)
        for p in range(pairs):
            bias = block_bias(own_bias, p) + causal
            scores = scores_of(r, p, kv_ref[r, :rows, columns(p)], bias)
            peak = jnp.maximum(jnp.max(scores, axis=1, keepdims=True), FLOOR)
            e = jnp.exp(scores - peak)
            top[p] = jnp.broadcast_to(peak, (2 * rows, 2 * HD))
            tot[p] = jnp.broadcast_to(jnp.sum(e, axis=1, keepdims=True), (2 * rows, 2 * HD))
            acc[p] = jnp.dot(
                e.astype(jnp.bfloat16), kv_ref[r, :rows, value_columns(p)],
                preferred_element_type=jnp.float32,
            )

        def chunk(j, carry):
            pool_rows(items[r, j], j)
            bias = chunk_bias(r, j)
            for p in range(pairs):
                scores = scores_of(
                    r, p, items[r, j, :rows, columns(p)], block_bias(bias, p)
                )
                old = top[p]
                peak = jnp.maximum(old, jnp.max(scores, axis=1, keepdims=True))
                shrink = jnp.exp(old - peak)
                e = jnp.exp(scores - peak[:, :1])
                top[p] = peak
                tot[p] = tot[p] * shrink + jnp.sum(e, axis=1, keepdims=True)
                acc[p] = acc[p] * shrink + jnp.dot(
                    e.astype(jnp.bfloat16), items[r, j, :rows, value_columns(p)],
                    preferred_element_type=jnp.float32,
                )
            return carry

        lax.fori_loop(0, i, chunk, 0)

        pshape = (rows, shards * PAD)
        pslot = lax.broadcasted_iota(jnp.int32, pshape, 1)
        inner = pslot % PAD
        end = (pslot // PAD) * rows + inner * L_CMP + L_CMP - 1
        pos = i * rows + lax.broadcasted_iota(jnp.int32, pshape, 0)
        usable = (inner < rows // L_CMP) & (end <= pos) & (end < live_at(r))
        pbias = jnp.where(usable, 0.0, LOW)
        pbias = jnp.concatenate([pbias, pbias], 0)
        gates = g_ref[seq_at(r)]
        gate_pos = i * rows + lax.broadcasted_iota(jnp.int32, gates.shape, 0)
        gates = jnp.where(gate_pos < live_at(r), gates, 0.0)
        for p in range(pairs):
            scores = scores_of(r, p, pools[:, columns(p)], pbias)
            peak = jnp.maximum(jnp.max(scores, axis=1, keepdims=True), FLOOR)
            e = jnp.exp(scores - peak)
            total = jnp.sum(e, axis=1, keepdims=True)
            pooled = jnp.dot(
                e.astype(jnp.bfloat16), pools[:, value_columns(p)],
                preferred_element_type=jnp.float32,
            ) / jnp.where(total > 0, total, 1.0)
            picked_total = tot[p]
            picked = acc[p] / jnp.where(picked_total > 0, picked_total, 1.0)
            halves = []
            for side_at in range(2):
                h = 2 * p + side_at
                span = slice(side_at * rows, (side_at + 1) * rows)
                halves.append(
                    gates[:, h : h + 1] * pooled[span]
                    + gates[:, heads + h : heads + h + 1] * picked[span]
                )
            att[r, t, :, columns(p)] = jnp.where(first, halves[0], halves[1]).astype(
                jnp.bfloat16
            )

    def step(r, carry):
        @pl.when(r < mine)
        def _():
            def arrive(n, inner):
                j = i - 1 - n
                relay_copy(r, j).wait_recv()

                @pl.when(r < after)
                def _():
                    relay_copy(r, j).start()

                return inner

            lax.fori_loop(0, i, arrive, 0)

            @pl.when((i > 0) & (r + 1 < after))
            def _():
                own_copy(r + 1).start()

            attend(r)
            for d in range(1, chips):
                block_copy(r, d, t, side(d)).start()
            block_copy(r, 0, t, mate).start()

        @pl.when(r >= 1)
        def _():
            b = r - 1
            for d in range(1, chips):
                block_copy(b, d, origin(d) + c, mate).wait_recv()
                block_copy(b, chips - 1 + d, origin(d) + c, mate).start()
            block_copy(b, 0, mate, mate).wait_recv()
            for d in range(1, chips):
                block_copy(b, chips - 1 + d, origin(d) + 1 - c, mate).wait_recv()

            @pl.when(r == 1)
            def _():
                w_copy.wait()

            total = jnp.dot(att[b, 0], w_vmem[:width, :], preferred_element_type=jnp.float32)
            for g in range(1, ntp):
                total = total + jnp.dot(
                    att[b, g], w_vmem[g * width : (g + 1) * width, :],
                    preferred_element_type=jnp.float32,
                )
            mixed[b] = total.astype(jnp.bfloat16)
            for d in range(1, ntp):
                out_copy(b, d).start()
            out_ref[b, :, pl.ds(pl.multiple_of(t * col, col), col)] = mixed[
                b, pl.ds(pl.multiple_of(t * part, part), part), :
            ]

        return carry

    lax.fori_loop(0, mine + 1, step, 0)

    def blank(r, carry):
        out_ref[r] = jnp.zeros(out_ref.shape[1:], out_ref.dtype)
        return carry

    lax.fori_loop(mine, seqs, blank, 0)

    def finish(r, carry):
        for d in range(1, ntp):
            out_copy(r, d).wait_send()
            source = lax.rem(t + ntp - d, ntp)
            pltpu.make_async_remote_copy(
                src_ref=mixed.at[r, :part, :],
                dst_ref=out_ref.at[r, :, pl.ds(pl.multiple_of(source * col, col), col)],
                send_sem=o_send.at[r, d], recv_sem=o_recv.at[r, d],
                device_id={"tp": source}, device_id_type=MESH,
            ).wait_recv()
        block_copy(r, 0, t, mate).wait_send()
        for d in range(1, chips):
            block_copy(r, d, t, side(d)).wait_send()
            block_copy(r, chips - 1 + d, origin(d) + c, mate).wait_send()
        return carry

    lax.fori_loop(0, mine, finish, 0)

    parts = jnp.stack([out_ref[ranks[s]] for s in range(seqs)], 0)
    final_ref[...] = jnp.swapaxes(parts, 0, 1)

    def sent(r, carry):
        own_copy(r).wait_send()

        def relayed(j, inner):
            relay_copy(r, j).wait_send()
            return inner

        lax.fori_loop(0, i, relayed, 0)
        return carry

    lax.fori_loop(0, after, sent, 0)


def body(tokens, lengths, chosen, w_query, w_key, w_value, w_gate, pool_weights, w_out):
    rows, seqs, model = tokens.shape
    width = w_query.shape[1]
    heads = width // HD
    col = w_out.shape[1]
    shards = lax.axis_size("kv")
    ntp = lax.axis_size("tp")
    chips = ntp // 2
    blocks = rows // QB
    slots = rank_slots(seqs, rows * shards, rows, shards)
    steps = 4
    depth = model // steps

    pool = jnp.concatenate(
        [jnp.tile(pool_weights[0], (1, heads)), jnp.tile(pool_weights[1], (1, heads))], 1
    )
    listed = chosen.reshape(seqs, heads * blocks, chosen.shape[3])
    gate_w = w_gate.transpose(1, 2, 0).reshape(2 * heads, steps, depth).transpose(1, 0, 2)

    vmem = pl.BlockSpec(memory_space=pltpu.VMEM)
    smem = pl.BlockSpec(memory_space=pltpu.SMEM)
    anywhere = pl.BlockSpec(memory_space=pl.ANY)
    dma = pltpu.SemaphoreType.DMA
    bf16, f32 = jnp.bfloat16, jnp.float32
    state = pltpu.VMEM((heads // 2, 2 * rows, 2 * HD), f32)
    return pl.pallas_call(
        functools.partial(mixer_kernel, slots, shards, ntp),
        out_shape=jax.ShapeDtypeStruct((rows // ntp, seqs, ntp * col), bf16),
        in_specs=[smem] + [vmem] * 3 + [anywhere] * 5,
        out_specs=vmem,
        scratch_shapes=[
            pltpu.VMEM((steps, rows, seqs, depth), bf16),
            pltpu.VMEM((steps, seqs * rows, depth), bf16),
            pltpu.VMEM((seqs, rows, 2 * width), f32),
            pltpu.VMEM((seqs, rows, width), bf16),
            pltpu.VMEM((seqs, rows, 2 * width), bf16),
            pltpu.VMEM((seqs, rows, 2 * heads), f32),
            pltpu.VMEM((seqs, rows // ntp, ntp * col), bf16),
            pltpu.VMEM((seqs, shards, rows, 2 * width), bf16),
            pltpu.VMEM((seqs, ntp, rows, width), bf16),
            pltpu.VMEM((seqs, rows, col), bf16),
            pltpu.VMEM((shards * PAD, 2 * width), bf16),
            state,
            state,
            state,
            pltpu.VMEM(w_query.shape, bf16),
            pltpu.VMEM(w_key.shape, bf16),
            pltpu.VMEM(w_value.shape, bf16),
            pltpu.VMEM(w_out.shape, bf16),
            dma((steps, 3)),
            dma,
            dma,
            dma((seqs, shards)),
            dma((seqs, shards)),
            dma((seqs, 2 * chips)),
            dma((seqs, 2 * chips)),
            dma((seqs, ntp)),
            dma((seqs, ntp)),
        ],
        compiler_params=pltpu.CompilerParams(
            collective_id=0, has_side_effects=True, vmem_limit_bytes=60 * 2**20
        ),
    )(lengths, listed, pool, gate_w, tokens, w_query, w_key, w_value, w_out)


def solution(mesh):
    placed = (
        P("kv", "grp", None),
        P("grp"),
        P("grp", "tp", "kv", None),
        P(None, "tp"),
        P(None, "tp"),
        P(None, "tp"),
        P(None, None, "tp"),
        P(),
        P(None, "tp"),
    )
    return jax.shard_map(
        body, mesh=mesh, in_specs=placed, out_specs=P(("kv", "tp"), "grp", None), check_vma=False
    )
```

```python
import functools

import jax
import jax.numpy as jnp
from jax import lax
from jax.experimental import pallas as pl
from jax.experimental.pallas import tpu as pltpu
from jax.sharding import PartitionSpec as P

HD = 64
QB = 64
L_CMP = 32
PAD = 16
LOW = -1e30
FLOOR = -1e29
MESH = pl.DeviceIdType.MESH
NT = (((1,), (1,)), ((), ()))


def rank_slots(seq_count, seq_len, rows, shards):
    total = seq_count * seq_len * 3 // 8
    slots = []
    for r in range(seq_count):
        most = min(seq_len, (total - (seq_count - 1 - r)) // (r + 1))
        slots.append(min(shards, -(-most // rows)))
    return slots


def ranks_of(lens):
    ranks = []
    for s in range(len(lens)):
        place = jnp.int32(0)
        for o in range(len(lens)):
            if o != s:
                ahead = lens[o] >= lens[s] if o < s else lens[o] > lens[s]
                place = place + jnp.where(ahead, 1, 0)
        ranks.append(place)
    return ranks


def order_kernel(len_ref, ranked_ref, out_ref):
    seqs = ranked_ref.shape[0]
    ranks = ranks_of([len_ref[s] for s in range(seqs)])
    parts = jnp.stack([ranked_ref[ranks[s]] for s in range(seqs)], 0)
    out_ref[...] = jnp.swapaxes(parts, 0, 1)


def mixer_kernel(
    slots, shards, ntp,
    len_ref, chosen_ref, pool_in, tok_hbm, wq_hbm, wk_hbm, wv_hbm, wg_hbm, w_hbm,
    out_ref,
    tok, xt, proj, q_ref, kv_ref, g_ref, pool_ref, wg_ref,
    items, att, mixed, pools, acc, top, tot, wq_vmem, wk_vmem, wv_vmem, w_vmem,
    in_sem, v_sem, q_sem, g_sem, w_sem, z_send, z_recv, a_send, a_recv, o_send, o_recv,
):
    seqs, rows, width = q_ref.shape
    steps, _, _, depth = tok.shape
    heads = width // HD
    pairs = heads // 2
    blocks = rows // QB
    chips = ntp // 2
    col = w_hbm.shape[1]
    part = rows // ntp
    i = lax.axis_index("kv")
    t = lax.axis_index("tp")
    x, c = t // 2, t % 2
    mate = x * 2 + (1 - c)

    def span_of(k):
        return pl.ds(pl.multiple_of(k * depth, depth), depth)

    def input_copies(k):
        return (
            pltpu.make_async_copy(tok_hbm.at[:, :, span_of(k)], tok.at[k], in_sem.at[k, 0]),
            pltpu.make_async_copy(wk_hbm.at[span_of(k)], wk_vmem.at[span_of(k)], in_sem.at[k, 1]),
        )

    for k in range(steps):
        for copy in input_copies(k):
            copy.start()
    v_copy = pltpu.make_async_copy(wv_hbm, wv_vmem, v_sem)
    v_copy.start()
    g_copy = pltpu.make_async_copy(wg_hbm, wg_ref, g_sem)
    g_copy.start()
    q_copy = pltpu.make_async_copy(wq_hbm, wq_vmem, q_sem)
    q_copy.start()
    w_copy = pltpu.make_async_copy(w_hbm, w_vmem, w_sem)
    w_copy.start()
    pools[...] = jnp.zeros_like(pools)
    for n in range(2):
        pool_ref[:, n * width : (n + 1) * width] = jnp.concatenate([pool_in[n]] * heads, 1)

    lens = [len_ref[s] for s in range(seqs)]
    ranks = ranks_of(lens)

    def seq_at(r):
        found = jnp.int32(0)
        for s in range(1, seqs):
            found = found + jnp.where(ranks[s] == r, s, 0)
        return found

    def live_at(r):
        found = jnp.int32(0)
        for s in range(seqs):
            found = found + jnp.where(ranks[s] == r, lens[s], 0)
        return found

    def active(shard):
        count = 0
        for n in slots:
            count = count + jnp.where(shard < n, 1, 0)
        return count

    mine = active(i)
    after = active(i + 1)

    barrier = pltpu.get_barrier_semaphore()
    for d in range(1, ntp):
        pl.semaphore_signal(
            barrier, inc=1, device_id={"tp": lax.rem(t + d, ntp)}, device_id_type=MESH
        )

    @pl.when(i > 0)
    def _():
        pl.semaphore_signal(barrier, inc=1, device_id={"kv": i - 1}, device_id_type=MESH)

    @pl.when(i < shards - 1)
    def _():
        pl.semaphore_signal(barrier, inc=1, device_id={"kv": i + 1}, device_id_type=MESH)

    def project(k, carry):
        for copy in input_copies(k):
            copy.wait()
        piece = jnp.swapaxes(tok[k], 0, 1).reshape(seqs * rows, depth)
        xt[k] = piece
        accumulate(k, piece, wk_vmem, 0)
        return carry

    def accumulate(k, piece, w, n):
        product = jnp.dot(piece, w[span_of(k), :], preferred_element_type=jnp.float32)
        product = product.reshape(seqs, rows, width)
        span = slice(n * width, (n + 1) * width)

        @pl.when(k == 0)
        def _():
            proj[:, :, span] = product

        @pl.when(k > 0)
        def _():
            proj[:, :, span] += product

    def keep(n):
        span = slice(n * width, (n + 1) * width)

        def one(r, carry):
            kv_ref[r, :, span] = proj[seq_at(r), :, span].astype(jnp.bfloat16)
            return carry

        lax.fori_loop(0, seqs, one, 0)

    lax.fori_loop(0, steps, project, 0)
    keep(0)
    expected = ntp - 1 + jnp.where(i > 0, 1, 0) + jnp.where(i < shards - 1, 1, 0)
    pl.semaphore_wait(barrier, expected)

    def half(n):
        return slice(n * width, (n + 1) * width)

    def own_copy(r, n):
        return pltpu.make_async_remote_copy(
            src_ref=kv_ref.at[r, :, half(n)], dst_ref=items.at[r, i, :, half(n)],
            send_sem=z_send.at[r, i, n], recv_sem=z_recv.at[r, i, n],
            device_id={"kv": i + 1}, device_id_type=MESH,
        )

    def relay_copy(r, j, n):
        return pltpu.make_async_remote_copy(
            src_ref=items.at[r, j, :, half(n)], dst_ref=items.at[r, j, :, half(n)],
            send_sem=z_send.at[r, j, n], recv_sem=z_recv.at[r, j, n],
            device_id={"kv": i + 1}, device_id_type=MESH,
        )

    def block_copy(r, k, block, target):
        return pltpu.make_async_remote_copy(
            src_ref=att.at[r, block], dst_ref=att.at[r, block],
            send_sem=a_send.at[r, k], recv_sem=a_recv.at[r, k],
            device_id={"tp": target}, device_id_type=MESH,
        )

    def side(d):
        return lax.rem(x + d, chips) * 2 + c

    def origin(d):
        return lax.rem(x + chips - d, chips) * 2

    def out_copy(r, d):
        target = lax.rem(t + d, ntp)
        return pltpu.make_async_remote_copy(
            src_ref=mixed.at[r, pl.ds(pl.multiple_of(target * part, part), part), :],
            dst_ref=out_ref.at[r, :, pl.ds(pl.multiple_of(t * col, col), col)],
            send_sem=o_send.at[r, d], recv_sem=o_recv.at[r, d],
            device_id={"tp": target}, device_id_type=MESH,
        )

    @pl.when(after > 0)
    def _():
        own_copy(0, 0).start()

    @pl.when((i == 0) & (after > 1))
    def _():
        own_copy(1, 0).start()

    v_copy.wait()

    def project_values(k, carry):
        accumulate(k, xt[k], wv_vmem, 1)
        return carry

    lax.fori_loop(0, steps, project_values, 0)
    keep(1)

    @pl.when(after > 0)
    def _():
        own_copy(0, 1).start()

    @pl.when((i == 0) & (after > 1))
    def _():
        own_copy(1, 1).start()

    def send_own(r, carry):
        own_copy(r, 0).start()
        own_copy(r, 1).start()
        return carry

    lax.fori_loop(2, jnp.where(i == 0, after, 2), send_own, 0)

    g_copy.wait()
    q_copy.wait()

    def project_queries(k, carry):
        piece = xt[k]
        product = jnp.dot(piece, wq_vmem[span_of(k), :], preferred_element_type=jnp.float32)
        product = product.reshape(seqs, rows, width)
        gate = jnp.dot(piece, wg_ref[span_of(k), :], preferred_element_type=jnp.float32)
        gate = gate.reshape(seqs, rows, 2 * heads)

        @pl.when(k == 0)
        def _():
            proj[:, :, :width] = product
            g_ref[...] = gate

        @pl.when(k > 0)
        def _():
            proj[:, :, :width] += product
            g_ref[...] += gate

        return carry

    lax.fori_loop(0, steps, project_queries, 0)
    g_ref[...] = jax.nn.sigmoid(g_ref[...])

    def keep_queries(r, carry):
        q_ref[r] = proj[seq_at(r), :, :width].astype(jnp.bfloat16) * jnp.bfloat16(HD**-0.5)
        return carry

    lax.fori_loop(0, mine, keep_queries, 0)

    lane = lax.broadcasted_iota(jnp.int32, (rows, 2 * HD), 1)
    first = lane < HD

    def pair_queries(r, p):
        q = q_ref[r, :, p * 2 * HD : (p + 1) * 2 * HD]
        zero = jnp.zeros_like(q)
        return jnp.concatenate([jnp.where(first, q, zero), jnp.where(first, zero, q)], 0)

    def scores_of(r, p, keys, bias):
        scores = lax.dot_general(
            pair_queries(r, p), keys, NT, preferred_element_type=jnp.float32
        )
        return scores + bias

    def chunk_bias(r, j):
        listed = chosen_ref[seq_at(r)]
        key_at = j * rows + lax.broadcasted_iota(jnp.int32, (heads * blocks, rows), 1)
        key_blk = key_at // QB
        hit = listed[:, :1] == key_blk
        for n in range(1, listed.shape[1]):
            hit = hit | (listed[:, n : n + 1] == key_blk)
        return jnp.where(hit & (key_at < live_at(r)), 0.0, LOW)

    def block_bias(bias, p):
        lines = [
            jnp.broadcast_to(bias[n : n + 1, :], (QB, rows))
            for n in range(p * 2 * blocks, (p + 1) * 2 * blocks)
        ]
        return jnp.concatenate(lines, 0)

    def pool_rows(kv, j):
        grouped = kv.astype(jnp.float32).reshape(rows // L_CMP, L_CMP, 2 * width)
        pooled = (grouped * pool_ref[...][None]).sum(1)
        fill = jnp.zeros((PAD - rows // L_CMP, 2 * width), jnp.float32)
        pools[pl.ds(pl.multiple_of(j * PAD, PAD), PAD), :] = jnp.concatenate(
            [pooled, fill], 0
        ).astype(jnp.bfloat16)

    def columns(p):
        return slice(p * 2 * HD, (p + 1) * 2 * HD)

    def value_columns(p):
        return slice(width + p * 2 * HD, width + (p + 1) * 2 * HD)

    def attend_own(r):
        row = lax.broadcasted_iota(jnp.int32, (2 * rows, rows), 0)
        row = jnp.where(row >= rows, row - rows, row)
        key = lax.broadcasted_iota(jnp.int32, (2 * rows, rows), 1)
        causal = jnp.where(key <= row, 0.0, LOW)
        pool_rows(kv_ref[r], i)
        own_bias = chunk_bias(r, i)
        for p in range(pairs):
            bias = block_bias(own_bias, p) + causal
            scores = scores_of(r, p, kv_ref[r, :rows, columns(p)], bias)
            peak = jnp.maximum(jnp.max(scores, axis=1, keepdims=True), FLOOR)
            e = jnp.exp(scores - peak)
            top[p] = jnp.broadcast_to(peak, (2 * rows, 2 * HD))
            tot[p] = jnp.broadcast_to(jnp.sum(e, axis=1, keepdims=True), (2 * rows, 2 * HD))
            acc[p] = jnp.dot(
                e.astype(jnp.bfloat16), kv_ref[r, :rows, value_columns(p)],
                preferred_element_type=jnp.float32,
            )

    def attend(r):
        def chunk(j, carry):
            pool_rows(items[r, j], j)
            bias = chunk_bias(r, j)
            for p in range(pairs):
                scores = scores_of(
                    r, p, items[r, j, :rows, columns(p)], block_bias(bias, p)
                )
                old = top[p]
                peak = jnp.maximum(old, jnp.max(scores, axis=1, keepdims=True))
                shrink = jnp.exp(old - peak)
                e = jnp.exp(scores - peak[:, :1])
                top[p] = peak
                tot[p] = tot[p] * shrink + jnp.sum(e, axis=1, keepdims=True)
                acc[p] = acc[p] * shrink + jnp.dot(
                    e.astype(jnp.bfloat16), items[r, j, :rows, value_columns(p)],
                    preferred_element_type=jnp.float32,
                )
            return carry

        lax.fori_loop(0, i, chunk, 0)

        pshape = (rows, shards * PAD)
        pslot = lax.broadcasted_iota(jnp.int32, pshape, 1)
        inner = pslot % PAD
        end = (pslot // PAD) * rows + inner * L_CMP + L_CMP - 1
        pos = i * rows + lax.broadcasted_iota(jnp.int32, pshape, 0)
        usable = (inner < rows // L_CMP) & (end <= pos) & (end < live_at(r))
        pbias = jnp.where(usable, 0.0, LOW)
        pbias = jnp.concatenate([pbias, pbias], 0)
        gates = g_ref[seq_at(r)]
        gate_pos = i * rows + lax.broadcasted_iota(jnp.int32, gates.shape, 0)
        gates = jnp.where(gate_pos < live_at(r), gates, 0.0)
        for p in range(pairs):
            scores = scores_of(r, p, pools[:, columns(p)], pbias)
            peak = jnp.maximum(jnp.max(scores, axis=1, keepdims=True), FLOOR)
            e = jnp.exp(scores - peak)
            total = jnp.sum(e, axis=1, keepdims=True)
            pooled = jnp.dot(
                e.astype(jnp.bfloat16), pools[:, value_columns(p)],
                preferred_element_type=jnp.float32,
            ) / jnp.where(total > 0, total, 1.0)
            picked_total = tot[p]
            picked = acc[p] / jnp.where(picked_total > 0, picked_total, 1.0)
            halves = []
            for side_at in range(2):
                h = 2 * p + side_at
                span = slice(side_at * rows, (side_at + 1) * rows)
                halves.append(
                    gates[:, h : h + 1] * pooled[span]
                    + gates[:, heads + h : heads + h + 1] * picked[span]
                )
            att[r, t, :, columns(p)] = jnp.where(first, halves[0], halves[1]).astype(
                jnp.bfloat16
            )

    def step(r, carry):
        @pl.when(r < mine)
        def _():
            attend_own(r)

            def arrive(m, inner):
                j = i - 1 - m
                for n in range(2):
                    relay_copy(r, j, n).wait_recv()

                    @pl.when(r < after)
                    def _():
                        relay_copy(r, j, n).start()

                return inner

            lax.fori_loop(0, i, arrive, 0)

            @pl.when((i > 0) & (r + 1 < after))
            def _():
                own_copy(r + 1, 0).start()
                own_copy(r + 1, 1).start()

            attend(r)
            for d in range(1, chips):
                block_copy(r, d, t, side(d)).start()
            block_copy(r, 0, t, mate).start()

        @pl.when(r >= 1)
        def _():
            b = r - 1
            for d in range(1, chips):
                block_copy(b, d, origin(d) + c, mate).wait_recv()
                block_copy(b, chips - 1 + d, origin(d) + c, mate).start()
            block_copy(b, 0, mate, mate).wait_recv()
            for d in range(1, chips):
                block_copy(b, chips - 1 + d, origin(d) + 1 - c, mate).wait_recv()

            @pl.when(r == 1)
            def _():
                w_copy.wait()

            total = jnp.dot(att[b, 0], w_vmem[:width, :], preferred_element_type=jnp.float32)
            for g in range(1, ntp):
                total = total + jnp.dot(
                    att[b, g], w_vmem[g * width : (g + 1) * width, :],
                    preferred_element_type=jnp.float32,
                )
            mixed[b] = total.astype(jnp.bfloat16)
            for d in range(1, ntp):
                out_copy(b, d).start()
            out_ref[b, :, pl.ds(pl.multiple_of(t * col, col), col)] = mixed[
                b, pl.ds(pl.multiple_of(t * part, part), part), :
            ]

        return carry

    lax.fori_loop(0, mine + 1, step, 0)

    def blank(r, carry):
        out_ref[r] = jnp.zeros(out_ref.shape[1:], out_ref.dtype)
        return carry

    lax.fori_loop(mine, seqs, blank, 0)

    def finish(r, carry):
        for d in range(1, ntp):
            out_copy(r, d).wait_send()
            source = lax.rem(t + ntp - d, ntp)
            pltpu.make_async_remote_copy(
                src_ref=mixed.at[r, :part, :],
                dst_ref=out_ref.at[r, :, pl.ds(pl.multiple_of(source * col, col), col)],
                send_sem=o_send.at[r, d], recv_sem=o_recv.at[r, d],
                device_id={"tp": source}, device_id_type=MESH,
            ).wait_recv()
        block_copy(r, 0, t, mate).wait_send()
        for d in range(1, chips):
            block_copy(r, d, t, side(d)).wait_send()
            block_copy(r, chips - 1 + d, origin(d) + c, mate).wait_send()
        return carry

    lax.fori_loop(0, mine, finish, 0)

    def sent(r, carry):
        for n in range(2):
            own_copy(r, n).wait_send()

        def relayed(j, inner):
            for n in range(2):
                relay_copy(r, j, n).wait_send()
            return inner

        lax.fori_loop(0, i, relayed, 0)
        return carry

    lax.fori_loop(0, after, sent, 0)


def body(tokens, lengths, chosen, w_query, w_key, w_value, w_gate, pool_weights, w_out):
    rows, seqs, model = tokens.shape
    width = w_query.shape[1]
    heads = width // HD
    col = w_out.shape[1]
    shards = lax.axis_size("kv")
    ntp = lax.axis_size("tp")
    chips = ntp // 2
    blocks = rows // QB
    slots = rank_slots(seqs, rows * shards, rows, shards)
    steps = 4
    depth = model // steps

    listed = chosen.reshape(seqs, heads * blocks, chosen.shape[3])
    gate_w = w_gate.reshape(model, 2 * heads)

    vmem = pl.BlockSpec(memory_space=pltpu.VMEM)
    smem = pl.BlockSpec(memory_space=pltpu.SMEM)
    anywhere = pl.BlockSpec(memory_space=pl.ANY)
    dma = pltpu.SemaphoreType.DMA
    bf16, f32 = jnp.bfloat16, jnp.float32
    state = pltpu.VMEM((heads // 2, 2 * rows, 2 * HD), f32)
    ranked = pl.pallas_call(
        functools.partial(mixer_kernel, slots, shards, ntp),
        out_shape=jax.ShapeDtypeStruct((seqs, rows // ntp, ntp * col), bf16),
        in_specs=[smem] + [vmem] * 2 + [anywhere] * 6,
        out_specs=vmem,
        scratch_shapes=[
            pltpu.VMEM((steps, rows, seqs, depth), bf16),
            pltpu.VMEM((steps, seqs * rows, depth), bf16),
            pltpu.VMEM((seqs, rows, 2 * width), f32),
            pltpu.VMEM((seqs, rows, width), bf16),
            pltpu.VMEM((seqs, rows, 2 * width), bf16),
            pltpu.VMEM((seqs, rows, 2 * heads), f32),
            pltpu.VMEM((L_CMP, 2 * width), f32),
            pltpu.VMEM((model, 2 * heads), bf16),
            pltpu.VMEM((seqs, shards, rows, 2 * width), bf16),
            pltpu.VMEM((seqs, ntp, rows, width), bf16),
            pltpu.VMEM((seqs, rows, col), bf16),
            pltpu.VMEM((shards * PAD, 2 * width), bf16),
            state,
            state,
            state,
            pltpu.VMEM(w_query.shape, bf16),
            pltpu.VMEM(w_key.shape, bf16),
            pltpu.VMEM(w_value.shape, bf16),
            pltpu.VMEM(w_out.shape, bf16),
            dma((steps, 2)),
            dma,
            dma,
            dma,
            dma,
            dma((seqs, shards, 2)),
            dma((seqs, shards, 2)),
            dma((seqs, 2 * chips)),
            dma((seqs, 2 * chips)),
            dma((seqs, ntp)),
            dma((seqs, ntp)),
        ],
        compiler_params=pltpu.CompilerParams(
            collective_id=0, has_side_effects=True, vmem_limit_bytes=60 * 2**20
        ),
    )(lengths, listed, pool_weights, tokens, w_query, w_key, w_value, gate_w, w_out)
    part = rows // ntp
    tile = ntp * col // 4
    return pl.pallas_call(
        order_kernel,
        grid_spec=pltpu.PrefetchScalarGridSpec(
            num_scalar_prefetch=1,
            grid=(4,),
            in_specs=[pl.BlockSpec((seqs, part, tile), lambda k, *_: (0, 0, k))],
            out_specs=pl.BlockSpec((part, seqs, tile), lambda k, *_: (0, 0, k)),
        ),
        out_shape=jax.ShapeDtypeStruct((part, seqs, ntp * col), bf16),
    )(lengths, ranked)


def solution(mesh):
    placed = (
        P("kv", "grp", None),
        P("grp"),
        P("grp", "tp", "kv", None),
        P(None, "tp"),
        P(None, "tp"),
        P(None, "tp"),
        P(None, None, "tp"),
        P(),
        P(None, "tp"),
    )
    return jax.shard_map(
        body, mesh=mesh, in_specs=placed, out_specs=P(("kv", "tp"), "grp", None), check_vma=False
    )
```
